32 devices in a mesh: grp: 2 (over y), fs: 4 (over z), tp: 4 (over x, core).
Axes of the slice: x: 2, y: 2, z: 4, core: 2. Of those that a mesh axis runs over, the one named last changes fastest.
Arguments:
- tokens: bfloat16 [4096, 2048], P(('grp', 'fs')), parts along dimension 0, may hold values from -6 to 6
- norm_in: bfloat16 [2048], replicated, may hold values from 0.099609375 to 1.8984375
- w_value: bfloat16 [2048, 2048], P('fs', 'tp'), may hold values from -0.125 to 0.125
- w_gate: bfloat16 [2048, 2048], P('fs', 'tp'), may hold values from -0.125 to 0.125
- conv_kernel: float32 [31, 2048], replicated, as said below
- ln_gain: bfloat16 [2048], replicated, may hold values from 0.099609375 to 1.8984375
- ln_shift: bfloat16 [2048], replicated, may hold values from -3 to 3
- w_out: bfloat16 [2048, 2048], P('tp', 'fs'), may hold values from -0.125 to 0.125
- norm_mlp: bfloat16 [2048], replicated, may hold values from 0.099609375 to 1.8984375
- w_up: bfloat16 [2048, 8192], P('fs', 'tp'), may hold values from -0.125 to 0.125
- w_down: bfloat16 [8192, 2048], P('tp', 'fs'), may hold values from -0.0625 to 0.0625
Outputs:
- layer_out: bfloat16 [4096, 2048], P(('grp', 'fs', 'tp')), parts along dimension 0
The draws below stay inside these ranges and needn't reach their ends.
There are 2 independent parts, one for each index of `grp`. The reference program is written for one: setup_inputs(seed, part) draws one part's arguments, and reference() takes and returns one part's arrays. A program takes and returns all parts, laid end to end along the dimension named above; an argument that names none is the same for every part. Nothing has to cross between parts.
Inputs may be any that keep to these rules, and one draw needn't show every extreme that they name: `conv_kernel`: a depthwise kernel.
All inputs are finite; a program needn't handle non-finite values.
Results may differ from the reference program's by a relative error of at most 0.018.
Values may be sent and summed in bfloat16 or wider, within the bound.
No kernel may reach another device: no remote copies, remote signals or barrier semaphores. Data moves between devices by JAX's collectives and lax.ppermute only.
A program may use at most 64 MiB of HBM per device.

```python
import jax
import jax.numpy as jnp
from jax import lax

D = 2048
FF = 8192
KERNEL = 31
SEQ = 512
TOKENS = 2048
N_FS = 4
N_TP = 4


def draw_conv_kernel(key, part):
    first, second = jax.random.split(jax.random.fold_in(key, 11), 2)
    base = jnp.clip(jax.random.normal(first, (KERNEL, D), jnp.float32), -4.0, 4.0) / jnp.sqrt(jnp.float32(KERNEL))
    channel = jnp.arange(D, dtype=jnp.float32) / D
    rising = jnp.exp(jnp.log(3.0) * channel) * jax.random.uniform(second, (D,), jnp.float32, 0.6, 1.4)
    return (base * rising[None, :]).astype(jnp.float32)


def block_scale(key, shape, cuts, low, high):
    def one(position, blocks):
        draws = jax.random.uniform(jax.random.fold_in(jax.random.fold_in(key, 6), position), (blocks,), jnp.float32, low / len(cuts), high / len(cuts))
        return jnp.repeat(jnp.exp(draws), shape[position] // blocks).reshape((-1,) + (1,) * (len(shape) - position - 1))

    factor_of = one(*cuts[0])
    for cut in cuts[1:]:
        factor_of = factor_of * one(*cut)
    return factor_of


def normal_values(key, dims, spread, reach, shards=(), kind=jnp.bfloat16):
    result = spread * jax.random.normal(key, dims, jnp.float32)
    if shards:
        result = result * block_scale(key, dims, shards, -0.22, 0.18)
    return jnp.clip(result, -reach, reach).astype(kind)


def setup_inputs(seed: int = 0, part: int = 0) -> dict:
    seeds = jax.random.split(jax.random.key(seed), 12)
    part_keys = jax.random.split(jax.random.fold_in(seeds[11], part), 12)
    return {
        "tokens": normal_values(part_keys[0], (TOKENS, D), 1.0, 6.0, ((0, 4),)),
        "norm_in": jnp.clip(1.0 + 0.18 * jax.random.normal(seeds[1], (D,), jnp.float32), 0.099609375, 1.8984375).astype(jnp.bfloat16),
        "w_value": normal_values(seeds[2], (D, D), D ** -0.5, 0.125, ((0, 4), (1, 4))),
        "w_gate": normal_values(seeds[3], (D, D), D ** -0.5, 0.125, ((0, 4), (1, 4))),
        "conv_kernel": draw_conv_kernel(jax.random.fold_in(seeds[11], 71), part),
        "ln_gain": jnp.clip(1.0 + 0.18 * jax.random.normal(seeds[5], (D,), jnp.float32), 0.099609375, 1.8984375).astype(jnp.bfloat16),
        "ln_shift": normal_values(seeds[6], (D,), 0.5, 3.0),
        "w_out": normal_values(seeds[7], (D, D), D ** -0.5, 0.125, ((0, 4), (1, 4))),
        "norm_mlp": jnp.clip(1.0 + 0.18 * jax.random.normal(seeds[8], (D,), jnp.float32), 0.099609375, 1.8984375).astype(jnp.bfloat16),
        "w_up": normal_values(seeds[9], (D, FF), D ** -0.5, 0.125, ((0, 4), (1, 4))),
        "w_down": normal_values(seeds[10], (FF, D), FF ** -0.5, 0.0625, ((0, 4), (1, 4))),
    }


def rms_scale(values, gain):
    as_float = values.astype(jnp.float32)
    scaled = as_float * lax.rsqrt(lax.optimization_barrier(jnp.mean(as_float * as_float, axis=-1, keepdims=True)) + 1e-06)
    return scaled * gain.astype(jnp.float32)

def grouped_sum(left, right, groups):
    inner = left.shape[1] // groups
    partials = jnp.einsum('stc,tcd->std', left.reshape(left.shape[0], groups, inner).astype(jnp.float32), right.reshape(groups, inner, right.shape[1]).astype(jnp.float32), precision=lax.Precision.HIGHEST)
    rounded = lax.optimization_barrier(partials.astype(jnp.bfloat16))
    return lax.optimization_barrier(jnp.sum(rounded.astype(jnp.float32), axis=1))

def reference(tokens, norm_in, w_value, w_gate, conv_kernel, ln_gain, ln_shift, w_out, norm_mlp, w_up, w_down):

    def one_sequence(sequence):
        normed_in = rms_scale(sequence, norm_in).astype(jnp.bfloat16)
        values_f = jnp.dot(normed_in, w_value, preferred_element_type=jnp.float32)
        gate_act = jnp.dot(normed_in, w_gate, preferred_element_type=jnp.float32)
        gated = values_f * jax.nn.sigmoid(gate_act)
        padded = jnp.pad(gated, ((KERNEL - 1, 0), (0, 0)))
        convolved = jnp.zeros_like(gated)
        for tap_index in range(KERNEL):
            convolved = convolved + conv_kernel[tap_index][None, :] * padded[tap_index:tap_index + SEQ]
        chan_mean = lax.optimization_barrier(jnp.mean(convolved, axis=-1, keepdims=True))
        chan_msq = lax.optimization_barrier(jnp.mean(convolved * convolved, axis=-1, keepdims=True))
        variance = chan_msq - chan_mean * chan_mean
        normed = (convolved - chan_mean) * lax.rsqrt(variance + 1e-05)
        normed = normed * ln_gain.astype(jnp.float32) + ln_shift.astype(jnp.float32)
        activated = jax.nn.silu(normed).astype(jnp.bfloat16)
        mixed = grouped_sum(activated, w_out, N_TP)
        residual = sequence.astype(jnp.float32) + mixed
        normed_mlp = rms_scale(residual, norm_mlp).astype(jnp.bfloat16)
        up_act = jnp.dot(normed_mlp, w_up, preferred_element_type=jnp.float32)
        hidden = jnp.square(jax.nn.relu(up_act)).astype(jnp.bfloat16)
        return (residual + grouped_sum(hidden, w_down, N_TP)).astype(jnp.bfloat16)
    sequences = tokens.reshape(N_FS, SEQ, D)
    return lax.map(one_sequence, sequences).reshape(TOKENS, D)
```

```python
import jax
import jax.numpy as jnp
from jax import lax
from jax.sharding import PartitionSpec as P

CORES = 2


def rms_scale(values, gain):
    as_float = values.astype(jnp.float32)
    scaled = as_float * lax.rsqrt(jnp.mean(as_float * as_float, axis=-1, keepdims=True) + 1e-06)
    return scaled * gain.astype(jnp.float32)


def after(value, *others):
    return lax.optimization_barrier((value, *others))[0]


def shift(value, axis, by):
    size = lax.axis_size(axis)
    return lax.ppermute(value, axis, [(i, (i + by) % size) for i in range(size)])


def core_shift(value):
    size = lax.axis_size("tp")
    return lax.ppermute(value, "tp", [(i, i - i % CORES + (i + 1) % CORES) for i in range(size)])


def chip_shift(value, by):
    size = lax.axis_size("tp")
    return lax.ppermute(value, "tp", [(i, (i + by * CORES) % size) for i in range(size)])


def side_shift(value, by):
    half = lax.axis_size("fs") // 2
    pairs = [(i, i - i % half + (i % half + by) % half) for i in range(2 * half)]
    return lax.ppermute(value, "fs", pairs)


def spread(piece):
    groups = lax.axis_size("grp")
    y = lax.axis_index("grp")
    return [(y, piece)] + [((y - d) % groups, shift(piece, "grp", d)) for d in range(1, groups)]


def rows_of(array, index, count):
    return lax.dynamic_slice_in_dim(array, index * count, count, 0)


def shards(
    tokens, norm_in, w_value, w_gate, conv_kernel, ln_gain, ln_shift, w_out, norm_mlp, w_up, w_down
):
    seq_len, width = tokens.shape
    n, tp, groups = lax.axis_size("fs"), lax.axis_size("tp"), lax.axis_size("grp")
    half = n // 2
    chips = tp // CORES
    y, z, t = lax.axis_index("grp"), lax.axis_index("fs"), lax.axis_index("tp")
    core, chip, side = t % CORES, t // CORES, z // half
    taps = conv_kernel.shape[0]
    rows, cols = w_value.shape
    part = rows // groups
    own = seq_len // tp

    normed_in = rms_scale(tokens, norm_in).astype(jnp.bfloat16)

    def product(first, count, piece):
        left = lax.dynamic_slice_in_dim(normed_in, first, count, 1)
        return jnp.dot(left, piece, preferred_element_type=jnp.float32)

    sums = [product(z * rows, rows, w) for w in (w_value, w_gate)]
    ring = [rows_of(w, y, part) for w in (w_value, w_gate)]
    marks = []
    for k in range(1, n):
        ring = [shift(r, "fs", 1) for r in ring]
        marks.append(ring[-1])
        source = (z - k) % n
        for i in range(2):
            for place, piece in spread(ring[i]):
                sums[i] = sums[i] + product(source * rows + place * part, part, piece)
    values_f, gate_act = sums

    out_rows, out_cols = w_out.shape
    out_part = out_rows // groups
    whole_out = jnp.zeros((out_rows, out_cols * n), w_out.dtype)
    whole_out = lax.dynamic_update_slice(whole_out, w_out, (0, z * out_cols))
    piece = after(rows_of(w_out, y, out_part), marks[max(n - 3, 0)])
    out_marks = []
    for k in range(1, n):
        piece = shift(piece, "fs", 1)
        out_marks.append(piece)
        for place, block in spread(piece):
            whole_out = lax.dynamic_update_slice(
                whole_out, block, (place * out_part, ((z - k) % n) * out_cols)
            )

    hid = w_up.shape[1] // 2
    up_part = w_up.shape[0] // groups
    up_rows = rows_of(w_up, y, up_part)
    up_mine = lax.dynamic_slice_in_dim(up_rows, side * hid, hid, 1)
    up_theirs = lax.dynamic_slice_in_dim(up_rows, (1 - side) * hid, hid, 1)
    down_part = hid // groups
    down_cols = w_down.shape[1]
    down_mine = rows_of(w_down, side * groups + y, down_part)
    down_theirs = rows_of(w_down, (1 - side) * groups + y, down_part)

    whole_up = jnp.zeros((w_up.shape[0] * n, hid), w_up.dtype)
    whole_up = lax.dynamic_update_slice(
        whole_up, lax.dynamic_slice_in_dim(w_up, side * hid, hid, 1), (z * w_up.shape[0], 0)
    )
    whole_down = jnp.zeros((hid, down_cols * n), w_down.dtype)
    whole_down = lax.dynamic_update_slice(
        whole_down, rows_of(w_down, side, hid), (0, z * down_cols)
    )

    def gather_half(mine, theirs, place_block, whole):
        held = [mine, shift(theirs, "fs", half)]
        sources = [z, (z + half) % n]
        first = held[1]
        for place, block in spread(held[1]):
            whole = place_block(whole, sources[1], place, block)
        for k in range(1, half):
            held = [side_shift(h, 1) for h in held]
            for i, h in enumerate(held):
                at = z if i == 0 else (z + half) % n
                source = at - at % half + (at % half - k) % half
                for place, block in spread(h):
                    whole = place_block(whole, source, place, block)
        return whole, first

    def place_up(whole, source, place, block):
        return lax.dynamic_update_slice(
            whole, block, (source * w_up.shape[0] + place * up_part, 0)
        )

    def place_down(whole, source, place, block):
        return lax.dynamic_update_slice(whole, block, (place * down_part, source * down_cols))

    mark = out_marks[max(n - 3, 0)]
    up_mine, up_theirs = after(up_mine, mark), after(up_theirs, mark)
    whole_up, mark = gather_half(up_mine, up_theirs, place_up, whole_up)
    down_mine, down_theirs = after(down_mine, mark), after(down_theirs, mark)
    whole_down, mark = gather_half(down_mine, down_theirs, place_down, whole_down)

    gated = values_f * jax.nn.sigmoid(gate_act)
    kernel = lax.dynamic_slice_in_dim(conv_kernel, t * cols, cols, 1)
    padded = jnp.pad(gated, ((taps - 1, 0), (0, 0)))
    convolved = jnp.zeros_like(gated)
    for tap in range(taps):
        convolved = convolved + kernel[tap][None, :] * padded[tap : tap + seq_len]
    stats = lax.psum((jnp.sum(convolved, axis=1), jnp.sum(convolved * convolved, axis=1)), "tp")
    chan_mean = (stats[0] / width)[:, None]
    chan_msq = (stats[1] / width)[:, None]
    variance = chan_msq - chan_mean * chan_mean
    gain_part = lax.dynamic_slice_in_dim(ln_gain, t * cols, cols, 0).astype(jnp.float32)
    shift_part = lax.dynamic_slice_in_dim(ln_shift, t * cols, cols, 0).astype(jnp.float32)
    normed = (convolved - chan_mean) * lax.rsqrt(variance + 1e-05) * gain_part + shift_part
    activated = jax.nn.silu(normed).astype(jnp.bfloat16)
    partial = jnp.dot(activated, whole_out, preferred_element_type=jnp.float32).astype(jnp.bfloat16)

    partial = partial.reshape(chips, CORES, own, width)
    theirs = lax.dynamic_index_in_dim(partial, 1 - core, 1, keepdims=False)
    ours = lax.dynamic_index_in_dim(partial, core, 1, keepdims=False)
    ours = ours.astype(jnp.float32) + core_shift(theirs).astype(jnp.float32)
    mixed = lax.dynamic_index_in_dim(ours, chip, 0, keepdims=False)
    for d in range(1, chips):
        block = lax.dynamic_index_in_dim(ours, (chip + d) % chips, 0, keepdims=False)
        mixed = mixed + chip_shift(block.astype(jnp.bfloat16), d).astype(jnp.float32)
    residual = rows_of(tokens, t, own).astype(jnp.float32) + mixed
    normed_mlp = rms_scale(residual, norm_mlp).astype(jnp.bfloat16)

    def gather_blocks(block):
        blocks = [block] + [chip_shift(block, d) for d in range(1, chips)]
        whole = jnp.stack(blocks)
        return jnp.stack([whole, core_shift(whole)]).reshape(tp * own, width)

    def feed_forward(acts):
        up_act = jnp.dot(acts, whole_up, preferred_element_type=jnp.float32)
        hidden = jnp.square(jax.nn.relu(up_act)).astype(jnp.bfloat16)
        result = jnp.dot(hidden, whole_down, preferred_element_type=jnp.float32)
        return result.astype(jnp.bfloat16).reshape(CORES, chips, own, width)

    def reduce_blocks(blocks):
        ours = blocks[0].astype(jnp.float32) + core_shift(blocks[1]).astype(jnp.float32)
        total = ours[0]
        for d in range(1, chips):
            total = total + chip_shift(ours[d].astype(jnp.bfloat16), -d).astype(jnp.float32)
        return total

    pair_block = shift(normed_mlp, "fs", half)
    near = feed_forward(gather_blocks(normed_mlp))
    far = feed_forward(gather_blocks(pair_block))
    far_sum = shift(reduce_blocks(far).astype(jnp.bfloat16), "fs", half)
    total = reduce_blocks(near) + far_sum.astype(jnp.float32)
    return (residual + total).astype(jnp.bfloat16)


def solution(mesh):
    in_specs = (
        P(("grp", "fs"), None),
        P(),
        P("fs", "tp"),
        P("fs", "tp"),
        P(),
        P(),
        P(),
        P("tp", "fs"),
        P(),
        P("fs", "tp"),
        P("tp", "fs"),
    )
    out_specs = P(("grp", "fs", "tp"), None)
    return jax.shard_map(shards, mesh=mesh, in_specs=in_specs, out_specs=out_specs, check_vma=False)
```

```python
import functools

import jax
import jax.numpy as jnp
from jax import lax
from jax.experimental import pallas as pl
from jax.experimental.pallas import tpu as pltpu
from jax.sharding import PartitionSpec as P

CORES = 2


def rms_scale(values, gain):
    as_float = values.astype(jnp.float32)
    scaled = as_float * lax.rsqrt(jnp.mean(as_float * as_float, axis=-1, keepdims=True) + 1e-06)
    return scaled * gain.astype(jnp.float32)


def after(value, *others):
    return lax.optimization_barrier((value, *others))[0]


def shift(value, axis, by):
    size = lax.axis_size(axis)
    return lax.ppermute(value, axis, [(i, (i + by) % size) for i in range(size)])


def core_shift(value):
    size = lax.axis_size("tp")
    return lax.ppermute(value, "tp", [(i, i - i % CORES + (i + 1) % CORES) for i in range(size)])


def chip_shift(value, by):
    size = lax.axis_size("tp")
    return lax.ppermute(value, "tp", [(i, (i + by * CORES) % size) for i in range(size)])


def side_shift(value, by):
    half = lax.axis_size("fs") // 2
    pairs = [(i, i - i % half + (i % half + by) % half) for i in range(2 * half)]
    return lax.ppermute(value, "fs", pairs)


def spread(piece):
    groups = lax.axis_size("grp")
    return [piece] + [shift(piece, "grp", d) for d in range(1, groups)]


def rows_of(array, index, count):
    return lax.dynamic_slice_in_dim(array, index * count, count, 0)


ANY = pl.BlockSpec(memory_space=pl.ANY)
VMEM = pl.BlockSpec(memory_space=pltpu.VMEM)
BF16, F32 = jnp.bfloat16, jnp.float32


def call(body, operands, specs, outs, scratch, flops, copied):
    moved = sum(o.size * o.dtype.itemsize for o in operands)
    return pl.pallas_call(
        body,
        out_shape=outs,
        in_specs=specs,
        out_specs=jax.tree.map(lambda _: VMEM, outs),
        scratch_shapes=scratch,
        compiler_params=pltpu.CompilerParams(vmem_limit_bytes=44 << 20),
        cost_estimate=pl.CostEstimate(flops=flops, bytes_accessed=moved, transcendentals=0),
    )(*operands)


def at(start, count):
    return pl.ds(pl.multiple_of(start, 16), count)


def lanes(start, count):
    return pl.ds(pl.multiple_of(start, 128), count)


def row_of_grp(d):
    groups = lax.axis_size("grp")
    return lax.rem(lax.axis_index("grp") + groups - d, groups)


def ring_source(k):
    n = lax.axis_size("fs")
    return lax.rem(lax.axis_index("fs") + n - k, n)


def side_source(k, across):
    n = lax.axis_size("fs")
    half = n // 2
    z = lax.axis_index("fs")
    side = lax.div(z, half)
    side = 1 - side if across else side
    return side * half + lax.rem(lax.rem(z, half) + half - k, half)


def start_all(copies, sems):
    made = [pltpu.make_async_copy(s, d, sems.at[i]) for i, (s, d) in enumerate(copies)]
    for copy in made:
        copy.start()
    return made


def project_kernel(n, groups, taps, tokens, gain, kernel, *refs):
    per = 1 + (n - 1) * groups
    values, gates = refs[:per], refs[per : 2 * per]
    conv, stats, weights, normed, gated, sums, sems = refs[2 * per :]
    seq, width = tokens.shape
    rows, cols = values[0].shape
    part = rows // groups
    copies = []
    for i, pieces in enumerate((values, gates)):
        columns = pl.ds(i * cols, cols)
        copies.append((pieces[0], weights.at[at(ring_source(0) * rows, rows), columns]))
        for k in range(1, n):
            for d in range(groups):
                start = ring_source(k) * rows + row_of_grp(d) * part
                piece = pieces[1 + (k - 1) * groups + d]
                copies.append((piece, weights.at[at(start, part), columns]))
    made = start_all(copies, sems)
    step = 64

    @pl.loop(0, seq // step)
    def _(i):
        block = pl.ds(pl.multiple_of(i * step, step), step)
        x = tokens[block, :].astype(F32)
        x = x * lax.rsqrt(jnp.mean(x * x, axis=-1, keepdims=True) + 1e-06)
        normed[block, :] = (x * gain[...]).astype(BF16)

    pad = 32
    gated[:, 0:pad, :] = jnp.zeros((cols // 128, pad, 128), F32)
    sums[...] = jnp.zeros_like(sums)
    for copy in made:
        copy.wait()
    tile = min(256, cols)
    for j in range(cols // tile):
        v = jnp.dot(normed[...], weights[:, j * tile : (j + 1) * tile], preferred_element_type=F32)
        g = jnp.dot(
            normed[...],
            weights[:, cols + j * tile : cols + (j + 1) * tile],
            preferred_element_type=F32,
        )
        v = v * jax.nn.sigmoid(g)
        for i in range(tile // 128):
            gated[j * (tile // 128) + i, pad : pad + seq, :] = v[:, i * 128 : (i + 1) * 128]

    @pl.loop(0, cols // 128)
    def _(j):
        for base in range(0, seq, step):
            total = jnp.zeros((step, 128), F32)
            for tap in range(taps):
                first = base + pad - taps + 1 + tap
                total += kernel[j, tap : tap + 1, :] * gated[j, first : first + step, :]
            block = slice(base, base + step)
            conv[j, block, :] = total
            sums[0, block, :] += total
            sums[1, block, :] += total * total

    ones = jnp.ones((8, 128), F32)
    for i in range(2):
        row = lax.dot_general(
            ones, sums[i], (((1,), (1,)), ((), ())), precision=lax.Precision.HIGHEST,
            preferred_element_type=F32,
        )
        stats[i : i + 1, :] = row[0:1, :]


def project(tokens, gain, kernel, values, gates):
    seq, width = tokens.shape
    rows, cols = values[0].shape
    n, groups = lax.axis_size("fs"), lax.axis_size("grp")
    taps = kernel.shape[0]
    kernel = kernel.reshape(taps, cols // 128, 128).transpose(1, 0, 2)
    count = len(values) + len(gates)
    return call(
        functools.partial(project_kernel, n, groups, taps),
        [tokens, gain, kernel, *values, *gates],
        [VMEM, VMEM, VMEM] + [ANY] * count,
        [
            jax.ShapeDtypeStruct((cols // 128, seq, 128), F32),
            jax.ShapeDtypeStruct((2, seq), F32),
        ],
        [
            pltpu.VMEM((width, 2 * cols), BF16),
            pltpu.VMEM((seq, width), BF16),
            pltpu.VMEM((cols // 128, seq + 32, 128), F32),
            pltpu.VMEM((2, seq, 128), F32),
            pltpu.SemaphoreType.DMA((count,)),
        ],
        4 * seq * width * cols,
        0,
    )


def mix_kernel(n, groups, width, conv, stats, gain, bias, *refs):
    per = 1 + (n - 1) * groups
    pieces = refs[:per]
    theirs, ours, weights, acts, spread_stats, sems = refs[per:]
    seq, cols = conv.shape[1], conv.shape[0] * 128
    piece_cols = pieces[0].shape[1]
    part = cols // groups
    copies = [(pieces[0], weights.at[:, lanes(ring_source(0) * piece_cols, piece_cols)])]
    for k in range(1, n):
        for d in range(groups):
            columns = lanes(ring_source(k) * piece_cols, piece_cols)
            piece = pieces[1 + (k - 1) * groups + d]
            copies.append((piece, weights.at[at(row_of_grp(d) * part, part), columns]))
    made = start_all(copies, sems)
    tp = lax.axis_size("tp")
    core = lax.rem(lax.axis_index("tp"), CORES)
    own = seq // tp
    chips = tp // CORES
    rows = lax.broadcasted_iota(jnp.int32, (2, 128), 0)
    for i in range(2):
        pick = jnp.where(rows == i, 1.0, 0.0).astype(F32)
        spread_stats[i] = lax.dot_general(
            stats[...], pick, (((0,), (0,)), ((), ())), precision=lax.Precision.HIGHEST,
            preferred_element_type=F32,
        ) / width
    for place in range(2):
        for chip in range(chips):
            source = (chip * CORES + (core if place else 1 - core)) * own
            block = at(source, own)
            mean = spread_stats[0, block, :]
            scale = lax.rsqrt(spread_stats[1, block, :] - mean * mean + 1e-05)
            for j in range(cols // 128):
                lane = slice(j * 128, (j + 1) * 128)
                v = (conv[j, block, :] - mean) * scale * gain[:, lane] + bias[:, lane]
                target = (place * chips + chip) * own
                acts[target : target + own, lane] = (v / (1.0 + jnp.exp(-v))).astype(BF16)
    for copy in made:
        copy.wait()
    tile = min(512, width)
    for place, out in enumerate((theirs, ours)):
        left = acts[place * chips * own : (place + 1) * chips * own, :]
        for j in range(width // tile):
            lane = slice(j * tile, (j + 1) * tile)
            out[:, lane] = jnp.dot(left, weights[:, lane], preferred_element_type=F32).astype(BF16)


def mix(conv, stats, gain, bias, pieces, width):
    seq, cols = conv.shape[1], conv.shape[0] * 128
    n, groups = lax.axis_size("fs"), lax.axis_size("grp")
    half = jax.ShapeDtypeStruct((seq // CORES, width), BF16)
    return call(
        functools.partial(mix_kernel, n, groups, width),
        [conv, stats, gain, bias, *pieces],
        [VMEM] * 4 + [ANY] * len(pieces),
        [half, half],
        [
            pltpu.VMEM((cols, width), BF16),
            pltpu.VMEM((seq, cols), BF16),
            pltpu.VMEM((2, seq, 128), F32),
            pltpu.SemaphoreType.DMA((len(pieces),)),
        ],
        2 * seq * width * cols,
        0,
    )


def feed_kernel(half, groups, blocks, *refs):
    per = 2 + (2 * half - 1) * groups - 1
    acts_in = refs[:blocks]
    ups, downs = refs[blocks : blocks + per], refs[blocks + per : blocks + 2 * per]
    theirs, ours, acts, up, down, hidden, sems = refs[blocks + 2 * per :]
    own = acts_in[0].shape[0]
    hid, width = down.shape
    up_rows, down_cols = ups[0].shape[0], downs[0].shape[1]
    up_part, down_part = up_rows // groups, hid // groups
    side = lax.div(lax.axis_index("fs"), half)
    copies = [(a, acts.at[pl.ds(i * own, own), :]) for i, a in enumerate(acts_in)]
    here = lax.axis_index("fs")
    copies.append((ups[0].at[:, lanes(side * hid, hid)], up.at[at(here * up_rows, up_rows), :]))
    late = [(downs[0].at[at(side * hid, hid), :], down.at[:, lanes(here * down_cols, down_cols)])]
    i = 1
    for k, across in places(half):
        source = side_source(k, across)
        for d in range(groups):
            row = row_of_grp(d)
            copies.append((ups[i], up.at[at(source * up_rows + row * up_part, up_part), :]))
            columns = lanes(source * down_cols, down_cols)
            late.append((downs[i], down.at[at(row * down_part, down_part), columns]))
            i += 1
    made = start_all(copies + late, sems)
    for copy in made[: len(copies)]:
        copy.wait()
    tile = min(256, hid)
    for j in range(hid // tile):
        lane = slice(j * tile, (j + 1) * tile)
        x = jnp.dot(acts[...], up[:, lane], preferred_element_type=F32)
        x = jnp.maximum(x, 0.0)
        hidden[:, lane] = (x * x).astype(BF16)
    for copy in made[len(copies) :]:
        copy.wait()
    tile = min(256, width)
    rows = theirs.shape[0]
    for j in range(width // tile):
        lane = slice(j * tile, (j + 1) * tile)
        x = jnp.dot(hidden[...], down[:, lane], preferred_element_type=F32).astype(BF16)
        ours[:, lane] = x[:rows]
        theirs[:, lane] = x[rows:]


def places(half):
    return [(0, True)] + [(k, a) for k in range(1, half) for a in (False, True)]


def feed(acts, ups, downs, hid):
    own, width = acts[0].shape
    half, groups = lax.axis_size("fs") // 2, lax.axis_size("grp")
    rows = own * len(acts)
    out = jax.ShapeDtypeStruct((rows // CORES, width), BF16)
    return call(
        functools.partial(feed_kernel, half, groups, len(acts)),
        [*acts, *ups, *downs],
        [ANY] * (len(acts) + len(ups) + len(downs)),
        [out, out],
        [
            pltpu.VMEM((rows, width), BF16),
            pltpu.VMEM((width, hid), BF16),
            pltpu.VMEM((hid, width), BF16),
            pltpu.VMEM((rows, hid), BF16),
            pltpu.SemaphoreType.DMA((len(acts) + len(ups) + len(downs),)),
        ],
        4 * rows * width * hid,
        0,
    )


def shards(
    tokens, norm_in, w_value, w_gate, conv_kernel, ln_gain, ln_shift, w_out, norm_mlp, w_up, w_down
):
    seq_len, width = tokens.shape
    n, tp, groups = lax.axis_size("fs"), lax.axis_size("tp"), lax.axis_size("grp")
    half = n // 2
    chips = tp // CORES
    y, z, t = lax.axis_index("grp"), lax.axis_index("fs"), lax.axis_index("tp")
    chip, side = t // CORES, z // half
    rows, cols = w_value.shape
    part = rows // groups
    own = seq_len // tp

    values, gates = [w_value], [w_gate]
    ring = [rows_of(w, y, part) for w in (w_value, w_gate)]
    marks = []
    for k in range(1, n):
        ring = [shift(r, "fs", 1) for r in ring]
        marks.append(ring[-1])
        values += spread(ring[0])
        gates += spread(ring[1])

    outs = [w_out]
    piece = after(rows_of(w_out, y, w_out.shape[0] // groups), marks[max(n - 3, 0)])
    out_marks = []
    for k in range(1, n):
        piece = shift(piece, "fs", 1)
        out_marks.append(piece)
        outs += spread(piece)

    hid = w_up.shape[1] // 2
    up_rows = rows_of(w_up, y, w_up.shape[0] // groups)
    up_mine = lax.dynamic_slice_in_dim(up_rows, side * hid, hid, 1)
    up_theirs = lax.dynamic_slice_in_dim(up_rows, (1 - side) * hid, hid, 1)
    down_mine = rows_of(w_down, side * groups + y, hid // groups)
    down_theirs = rows_of(w_down, (1 - side) * groups + y, hid // groups)

    def gather_half(mine, theirs):
        held = [mine, shift(theirs, "fs", half)]
        first = held[1]
        found = spread(first)
        for k in range(1, half):
            held = [side_shift(h, 1) for h in held]
            for h in held:
                found += spread(h)
        return found, first

    mark = out_marks[max(n - 3, 0)]
    found, mark = gather_half(after(up_mine, mark), after(up_theirs, mark))
    ups = [w_up] + found
    found, mark = gather_half(after(down_mine, mark), after(down_theirs, mark))
    downs = [w_down] + found

    kernel = lax.dynamic_slice_in_dim(conv_kernel, t * cols, cols, 1)
    gain_part = lax.dynamic_slice_in_dim(ln_gain, t * cols, cols, 0).astype(F32)[None, :]
    shift_part = lax.dynamic_slice_in_dim(ln_shift, t * cols, cols, 0).astype(F32)[None, :]
    convolved, stats = project(tokens, norm_in.astype(F32)[None, :], kernel, values, gates)
    stats = lax.psum(stats, "tp")
    theirs, ours = mix(convolved, stats, gain_part, shift_part, outs, width)

    ours = (ours.astype(F32) + core_shift(theirs).astype(F32)).reshape(chips, own, width)
    mixed = lax.dynamic_index_in_dim(ours, chip, 0, keepdims=False)
    for d in range(1, chips):
        block = lax.dynamic_index_in_dim(ours, (chip + d) % chips, 0, keepdims=False)
        mixed = mixed + chip_shift(block.astype(BF16), d).astype(F32)
    residual = rows_of(tokens, t, own).astype(F32) + mixed
    normed_mlp = rms_scale(residual, norm_mlp).astype(BF16)

    def gather_blocks(block):
        blocks = [block] + [chip_shift(block, d) for d in range(1, chips)]
        return blocks + [core_shift(b) for b in blocks]

    def reduce_blocks(theirs, ours):
        ours = ours.astype(F32) + core_shift(theirs).astype(F32)
        total = ours[:own]
        for d in range(1, chips):
            block = ours[d * own : (d + 1) * own].astype(BF16)
            total = total + chip_shift(block, -d).astype(F32)
        return total

    pair_block = shift(normed_mlp, "fs", half)
    near = feed(gather_blocks(normed_mlp), ups, downs, hid)
    far = feed(gather_blocks(pair_block), ups, downs, hid)
    far_sum = shift(reduce_blocks(*far).astype(BF16), "fs", half)
    total = reduce_blocks(*near) + far_sum.astype(F32)
    return (residual + total).astype(BF16)


def solution(mesh):
    in_specs = (
        P(("grp", "fs"), None),
        P(),
        P("fs", "tp"),
        P("fs", "tp"),
        P(),
        P(),
        P(),
        P("tp", "fs"),
        P(),
        P("fs", "tp"),
        P("tp", "fs"),
    )
    out_specs = P(("grp", "fs", "tp"), None)
    return jax.shard_map(shards, mesh=mesh, in_specs=in_specs, out_specs=out_specs, check_vma=False)
```
